32 devices in a mesh: sp: 4 (over z), dp: 8 (over y, x, core).
Axes of the slice: x: 2, y: 2, z: 4, core: 2. Of those that a mesh axis runs over, the one named last changes fastest.
Arguments:
- hidden: bfloat16 [8, 512, 2048], P('dp', 'sp'), may hold values from -6 to 6
- queries: bfloat16 [8, 512, 1024], P('dp', 'sp'), may hold values from -6 to 6
- values: bfloat16 [8, 512, 2048], P('dp', 'sp'), may hold values from -6 to 6
- key_weight: bfloat16 [2048, 1024], P('dp'), may hold values from -0.125 to 0.125
- decay_down: bfloat16 [2048, 16], replicated, may hold values from -0.125 to 0.125
- decay_up: float32 [16, 1024], replicated, may hold values from -1.5 to 1.5
- decay_bias: float32 [1024], replicated, may hold values from -1 to 8
- span_shift: bfloat16 [8, 512], P('dp', 'sp'), may hold values from -1.5 to 1.5, as said below
- norm_gain: float32 [2048], replicated, may hold values from 0.1 to 1.9
Outputs:
- attended: bfloat16 [8, 512, 2048], P('dp', 'sp')
The draws below stay inside these ranges and needn't reach their ends.
Inputs may be any that keep to these rules, and one draw needn't show every extreme that they name: `span_shift`: constant over each aligned block of 64 positions.
All inputs are finite; a program needn't handle non-finite values.
Results may differ from the reference program's by a relative error of at most 0.0073.
Values may be sent and summed in bfloat16 or wider, within the bound.
A program may use at most 64 MiB of HBM per device.

```python
import jax
import jax.numpy as jnp
from jax import lax

D = 2048
HEADS = 4
DK = 256
DV = 512
RANK = 16
BLOCK = 64
KEY = 1024
VAL = 2048
LENGTH = 512
BATCH = 8


def draw_decay_bias(key, part):
    pick_key, slow_key, fast_key = jax.random.split(jax.random.fold_in(key, 11), 3)
    share = 5
    slow_pick = jax.random.randint(pick_key, (KEY,), 0, 10) < share
    slow_value = jax.random.uniform(slow_key, (KEY,), jnp.float32, 6.0, 8.0)
    fast_value = jax.random.uniform(fast_key, (KEY,), jnp.float32, -1.0, 0.5)
    return jnp.where(slow_pick, slow_value, fast_value).astype(jnp.float32)


def draw_span_shift(key, part):
    level_key, sign_key = jax.random.split(jax.random.fold_in(key, 23), 2)
    blocks = LENGTH // BLOCK
    levels = jax.random.uniform(level_key, (BATCH, blocks), jnp.float32, -1.5, 1.5)
    return jnp.repeat(levels, BLOCK, axis=1).astype(jnp.bfloat16)


def steps_of(key, shape, cuts, low, top_value):
    loudness, own = 1.0, jax.random.fold_in(key, 6)
    for dim, shards_of in cuts:
        heights = jnp.exp(jax.random.uniform(jax.random.fold_in(own, dim), (shards_of,), jnp.float32, low / len(cuts), top_value / len(cuts)))
        loudness = loudness * jnp.repeat(heights, shape[dim] // shards_of).reshape([-1 if axis == dim else 1 for axis in range(len(shape))])
    return loudness


def gaussian(own_key, shape, spread, reach, cuts=(), dtype=jnp.bfloat16):
    values = jax.random.normal(own_key, shape, jnp.float32) * spread
    if len(cuts) > 0:
        values = steps_of(own_key, shape, cuts, -0.22, 0.18) * values
    return jnp.clip(values, min=-reach, max=reach).astype(dtype)


def setup_inputs(seed: int = 0) -> dict:
    splits = jax.random.split(jax.random.key(seed), 10)
    hidden = gaussian(splits[0], (BATCH, LENGTH, D), 1.0, 6.0, ((0, 8), (1, 4)))
    queries = gaussian(splits[1], (BATCH, LENGTH, KEY), 1.0, 6.0, ((0, 8), (1, 4)))
    values = gaussian(splits[2], (BATCH, LENGTH, VAL), 1.0, 6.0, ((0, 8), (1, 4)))
    key_weight = gaussian(splits[3], (D, KEY), D ** -0.5, 0.125, ((0, 8),))
    decay_down = gaussian(splits[4], (D, RANK), D ** -0.5, 0.125)
    decay_up = gaussian(splits[5], (RANK, KEY), RANK ** -0.5, 1.5, (), jnp.float32)
    decay_bias = draw_decay_bias(jax.random.fold_in(splits[9], 71), 0)
    span_shift = draw_span_shift(jax.random.fold_in(splits[9], 71), 0)
    norm_gain = jnp.clip(1.0 + 0.18 * jax.random.normal(splits[8], (VAL,), jnp.float32), 0.1, 1.9)
    return dict(hidden=hidden, queries=queries, values=values, key_weight=key_weight, decay_down=decay_down, decay_up=decay_up, decay_bias=decay_bias, span_shift=span_shift, norm_gain=norm_gain)


decay_tau = 16.0
norm_eps = 1e-05
highest = lax.Precision.HIGHEST

def mechanism(query, keys_in, value_in, log_decay):
    length, key_width = query.shape
    value_width = value_in.shape[-1]
    blocks = length // BLOCK
    step_decay = log_decay.reshape(blocks, BLOCK, key_width)
    inclusive = jnp.cumsum(step_decay, axis=1)
    exclusive = inclusive - step_decay
    total = inclusive[:, -1, :]
    query3 = query.reshape(blocks, BLOCK, key_width)
    keys3 = keys_in.reshape(blocks, BLOCK, key_width)
    value_tensor3 = value_in.reshape(blocks, BLOCK, value_width)
    query_forward_part = (query3 * jnp.exp(inclusive)).astype(jnp.bfloat16)
    key_fwd = (keys3 * jnp.exp(-inclusive)).astype(jnp.bfloat16)
    query_reverse_part = (query3 * jnp.exp(-exclusive)).astype(jnp.bfloat16)
    key_bwd = (keys3 * jnp.exp(exclusive)).astype(jnp.bfloat16)
    key_end = (keys3 * jnp.exp(total[:, None, :] - inclusive)).astype(jnp.bfloat16)
    fwd_scores = jnp.einsum('nid,njd->nij', query_forward_part, key_fwd, preferred_element_type=jnp.float32)
    bwd_scores = jnp.einsum('nid,njd->nij', query_reverse_part, key_bwd, preferred_element_type=jnp.float32)
    row_index = lax.broadcasted_iota(jnp.int32, (BLOCK, BLOCK), 0)
    col_index = lax.broadcasted_iota(jnp.int32, (BLOCK, BLOCK), 1)
    attention_scores = jnp.where((col_index <= row_index)[None], fwd_scores, bwd_scores).astype(jnp.bfloat16)
    inner_block_term = jnp.einsum('ucy,uyh->uch', attention_scores, value_tensor3, preferred_element_type=jnp.float32)
    end_terms = jnp.einsum('njd,nje->nde', key_end, value_tensor3, preferred_element_type=jnp.float32)
    start_terms = jnp.einsum('njd,nje->nde', key_bwd, value_tensor3, preferred_element_type=jnp.float32)
    rates = jnp.exp(total)

    def forward_step(carry_state, inputs):
        rate, term = inputs
        return (rate[:, None] * carry_state + term, carry_state)

    def backward_step(carry_state, inputs):
        rate, term = inputs
        state_here = rate[:, None] * carry_state
        return (state_here + term, state_here)
    empty = jnp.zeros((key_width, value_width), jnp.float32)
    _, forward_scan_states = lax.scan(forward_step, empty, (rates, end_terms))
    _, reverse_scan_states = lax.scan(backward_step, empty, (rates, start_terms), reverse=True)
    produced_rows = jnp.einsum('tzv,tvg->tzg', query_forward_part, forward_scan_states.astype(jnp.bfloat16), preferred_element_type=jnp.float32)
    produced_rows = produced_rows + jnp.einsum('tzv,tvg->tzg', query_reverse_part, reverse_scan_states.astype(jnp.bfloat16), preferred_element_type=jnp.float32)
    return (inner_block_term + produced_rows).reshape(length, value_width).astype(jnp.bfloat16)

def head_norm(mixed, gain):
    rows = mixed.shape[0]
    grouped = mixed.astype(jnp.float32).reshape(rows, HEADS, DV)
    normed = grouped * lax.rsqrt(lax.optimization_barrier(jnp.mean(grouped * grouped, axis=-1, keepdims=True)) + norm_eps)
    return (normed * gain.reshape(HEADS, DV)[None]).reshape(rows, VAL).astype(jnp.bfloat16)

def reference(hidden, queries, values, key_weight, decay_down, decay_up, decay_bias, span_shift, norm_gain):
    token_rows = hidden.reshape(-1, D)
    keys = jnp.dot(token_rows, key_weight, preferred_element_type=jnp.float32).astype(jnp.bfloat16).reshape(BATCH, LENGTH, KEY)
    low = jnp.dot(token_rows, decay_down, preferred_element_type=jnp.float32).astype(jnp.bfloat16).reshape(BATCH, LENGTH, RANK)

    def per_sequence(inputs):
        query_seq, keys_seq, value_seq, low_seq, shift_seq = inputs
        pre = jnp.dot(low_seq.astype(jnp.float32), decay_up, precision=highest, preferred_element_type=jnp.float32)
        pre = pre + decay_bias[None, :] + shift_seq.astype(jnp.float32)[:, None]
        log_decay = jax.nn.log_sigmoid(pre) / decay_tau

        def by_head(tensor, width):
            return tensor.reshape(LENGTH, HEADS, width).transpose(1, 0, 2)
        scaled = by_head(query_seq, DK).astype(jnp.float32) * DK ** (-0.5)
        mixed = jax.vmap(mechanism)(scaled, by_head(keys_seq, DK).astype(jnp.float32), by_head(value_seq, DV), by_head(log_decay, DK))
        return head_norm(mixed.transpose(1, 0, 2).reshape(LENGTH, VAL), norm_gain)
    return lax.map(per_sequence, (queries, keys, values, low, span_shift))
```

```python
import functools

import jax
import jax.numpy as jnp
from jax import lax
from jax.experimental import pallas as pl
from jax.experimental.pallas import tpu as pltpu
from jax.sharding import PartitionSpec as P

HEADS = 4
DK = 256
DV = 512
BLOCK = 64
KEY = 1024
VAL = 2048
CORES = 2
SPLIT = 2
DVS = DV // SPLIT

decay_tau = 16.0
norm_eps = 1e-05
highest = lax.Precision.HIGHEST
MESH = pl.DeviceIdType.MESH
f32 = jnp.float32
bf16 = jnp.bfloat16


def each(low, high, fn):
    if high - low <= 4:
        for j in range(low, high):
            fn(j)
    else:
        lax.fori_loop(low, high, lambda j, c: (fn(j), c)[1], 0)


def dot_nt(a, b):
    return lax.dot_general(a, b, (((1,), (1,)), ((), ())), preferred_element_type=f32)


def dot_tn(a, b):
    return lax.dot_general(a, b, (((0,), (0,)), ((), ())), preferred_element_type=f32)


def kernel(
    n_sp, n_dp,
    hid, que, val, kw, down, up, bias, shift, gain,
    out,
    wbuf, hv, qv, vv, outv, qf, qb, qx, qs, fac, rate, local, sbuf, rbuf, acc,
    lsem, osem, wsend, wrecv, psend, precv, csend, crecv,
):
    sp = lax.axis_index("sp")
    dp = lax.axis_index("dp")
    chips = n_dp // CORES
    chip = dp // CORES
    core = dp % CORES
    partner = chip * CORES + (1 - core)
    tok = hv.shape[0]
    depth = kw.shape[0]

    def peer(j):
        return lax.rem(chip + j, chips) * CORES + core

    def source_chip(j):
        return lax.rem(chip - j + chips, chips)

    wlocal = [
        pltpu.make_async_copy(kw.at[:, pl.ds(h * DK, DK)], wbuf.at[h, dp], lsem.at[h])
        for h in range(HEADS)
    ]
    inputs = [
        pltpu.make_async_copy(a, b, lsem.at[HEADS + i])
        for i, (a, b) in enumerate(((hid, hv), (que, qv), (val, vv)))
    ]
    for c in wlocal + inputs:
        c.start()

    barrier = pltpu.get_barrier_semaphore()
    each(1, chips, lambda j: pl.semaphore_signal(
        barrier, inc=1, device_id={"dp": peer(j)}, device_id_type=MESH))
    pl.semaphore_signal(barrier, inc=1, device_id={"dp": partner}, device_id_type=MESH)

    for side in (1, n_sp - 1):
        pl.semaphore_signal(
            barrier, inc=1, device_id={"sp": lax.rem(sp + side, n_sp)}, device_id_type=MESH)
    pl.semaphore_wait(barrier, chips + 2)

    def wcopy(h, j):
        return pltpu.make_async_remote_copy(
            src_ref=wbuf.at[h, dp], dst_ref=wbuf.at[h, dp],
            send_sem=wsend.at[h, j], recv_sem=wrecv.at[h, j],
            device_id={"dp": peer(j)}, device_id_type=MESH)

    def wland(h, j):
        slot = wbuf.at[h, source_chip(j) * CORES + core]
        return pltpu.make_async_remote_copy(
            src_ref=slot, dst_ref=slot,
            send_sem=wsend.at[h, j], recv_sem=wrecv.at[h, j],
            device_id={"dp": peer(j)}, device_id_type=MESH)

    def pcopy(h, j):
        slot = wbuf.at[h, source_chip(j) * CORES + core]
        return pltpu.make_async_remote_copy(
            src_ref=slot, dst_ref=slot,
            send_sem=psend.at[h, j], recv_sem=precv.at[h, j],
            device_id={"dp": partner}, device_id_type=MESH)

    def pland(h, j):
        slot = wbuf.at[h, source_chip(j) * CORES + (1 - core)]
        return pltpu.make_async_remote_copy(
            src_ref=slot, dst_ref=slot,
            send_sem=psend.at[h, j], recv_sem=precv.at[h, j],
            device_id={"dp": partner}, device_id_type=MESH)

    for h in range(HEADS):
        wlocal[h].wait()
        each(1, chips, lambda j, h=h: wcopy(h, j).start())
        pcopy(h, 0).start()

    inputs[0].wait()
    low = dot_nt(hv[...], down[...]).astype(bf16)
    steps = shift[...].astype(f32)
    inputs[1].wait()
    row = lax.broadcasted_iota(jnp.int32, (tok, DK), 0)
    first = row < BLOCK
    ti = lax.broadcasted_iota(jnp.int32, (tok, tok), 0)
    tj = lax.broadcasted_iota(jnp.int32, (tok, tok), 1)
    same = (ti < BLOCK) == (tj < BLOCK)
    below = tj <= ti
    tri = jnp.where(same & below, 1.0, 0.0).astype(f32)
    for h in range(HEADS):
        cols = pl.ds(h * DK, DK)
        pre = jnp.dot(low.astype(f32), up[:, cols], precision=highest, preferred_element_type=f32)
        pre = pre + bias[:, cols] + jnp.where(first, steps[:, :1], steps[:, BLOCK:BLOCK + 1])
        logd = (jnp.minimum(pre, 0.0) - jnp.log1p(jnp.exp(-jnp.abs(pre)))) * (1.0 / decay_tau)
        incl = jnp.dot(tri, logd, precision=highest, preferred_element_type=f32)
        excl = incl - logd
        t0 = incl[BLOCK - 1:BLOCK, :]
        t1 = incl[tok - 1:tok, :]
        here = jnp.where(first, t0, t1)
        after = jnp.where(first, t1, 0.0)
        before = jnp.where(first, 0.0, t0)
        scaled = qv[:, cols].astype(f32) * DK ** (-0.5)
        qf[:, cols] = (scaled * jnp.exp(incl)).astype(bf16)
        qb[:, cols] = (scaled * jnp.exp(-excl)).astype(bf16)
        qx[:, cols] = (scaled * jnp.exp(here - excl)).astype(bf16)
        qs[0, :, cols] = (scaled * jnp.exp(incl + before)).astype(bf16)
        qs[1, :, cols] = (scaled * jnp.exp(here - excl + after)).astype(bf16)
        fac[0, :, cols] = jnp.exp(-incl)
        fac[1, :, cols] = jnp.exp(excl)
        fac[2, :, cols] = jnp.exp(here - incl)
        fac[3, :, cols] = jnp.exp(here - incl + after)
        fac[4, :, cols] = jnp.exp(excl + before)
        rate[:, cols] = jnp.exp(t0 + t1)
    inputs[2].wait()

    def chain(way, h, s):
        target = jnp.clip(sp + 1 - 2 * way, 0, n_sp - 1)
        return pltpu.make_async_remote_copy(
            src_ref=sbuf.at[way, h, s], dst_ref=rbuf.at[way, h, s],
            send_sem=csend.at[way, h, s], recv_sem=crecv.at[way, h, s],
            device_id={"sp": target}, device_id_type=MESH)

    def phase_keys(h):
        def relay(j):
            wland(h, j).wait_recv()
            pcopy(h, j).start()
        each(1, chips, relay)
        each(0, chips, lambda j: pland(h, j).wait_recv())
        cols = pl.ds(h * DK, DK)
        weights = wbuf[h].reshape(n_dp * depth, DK)
        keys = jnp.dot(hv[...], weights, preferred_element_type=f32).astype(bf16).astype(f32)
        v = vv[:, pl.ds(h * DV, DV)]
        k_fwd = (keys * fac[3, :, cols]).astype(bf16)
        k_bwd = (keys * fac[4, :, cols]).astype(bf16)
        for way, k in ((0, k_fwd), (1, k_bwd)):
            local[way, h] = dot_tn(v, k)

            @pl.when(sp == (0 if way == 0 else n_sp - 1))
            def _(way=way):
                for s in range(SPLIT):
                    sbuf[way, h, s] = local[way, h, pl.ds(s * DVS, DVS), :].astype(bf16)
                    chain(way, h, s).start()

        kf = (keys * fac[0, :, cols]).astype(bf16)
        kb = (keys * fac[1, :, cols]).astype(bf16)
        ke = (keys * fac[2, :, cols]).astype(bf16)
        query_f, query_b, query_x = qf[:, cols], qb[:, cols], qx[:, cols]
        lower = jnp.where(same, dot_nt(query_f, kf), dot_nt(query_f, ke))
        upper = jnp.where(same, dot_nt(query_b, kb), dot_nt(query_x, kb))
        scores = jnp.where(below, lower, upper).astype(bf16)
        acc[h] = jnp.dot(scores, v, preferred_element_type=f32)

    def phase_chain(way, h):
        cols = pl.ds(h * DK, DK)
        edge = way * (n_sp - 1)
        other = (1 - way) * (n_sp - 1)

        @pl.when(sp != edge)
        def _():
            for s in range(SPLIT):
                rows = pl.ds(s * DVS, DVS)
                chain(way, h, s).wait_recv()

                @pl.when(sp != other)
                def _(s=s, rows=rows):
                    state = rbuf[way, h, s].astype(f32) * rate[:, cols] + local[way, h, rows, :]
                    sbuf[way, h, s] = state.astype(bf16)
                    chain(way, h, s).start()

                acc[h, :, rows] += dot_nt(qs[way, :, cols], rbuf[way, h, s])

    def out_copy(h):
        cols = pl.ds(h * DV, DV)
        return pltpu.make_async_copy(outv.at[:, cols], out.at[:, cols], osem.at[h])

    def phase_out(h):
        cols = pl.ds(h * DV, DV)
        mixed = acc[h].astype(bf16).astype(f32)
        scale = lax.rsqrt(jnp.mean(mixed * mixed, axis=-1, keepdims=True) + norm_eps)
        outv[:, cols] = (mixed * scale * gain[:, cols]).astype(bf16)
        out_copy(h).start()

    near = jnp.where(sp * 2 < n_sp, 0, 1)
    far = 1 - near
    for step in range(HEADS + 2):
        if step < HEADS:
            phase_keys(step)
        if 0 <= step - 1 < HEADS:
            phase_chain(near, step - 1)
        if 0 <= step - 2 < HEADS:
            phase_chain(far, step - 2)
            phase_out(step - 2)

    for h in range(HEADS):
        each(1, chips, lambda j, h=h: wcopy(h, j).wait_send())
        each(0, chips, lambda j, h=h: pcopy(h, j).wait_send())
        for way in range(2):
            @pl.when(sp != (1 - way) * (n_sp - 1))
            def _(h=h, way=way):
                for s in range(SPLIT):
                    chain(way, h, s).wait_send()
        out_copy(h).wait()


def body(n_sp, n_dp, hidden, queries, values, key_weight, decay_down, decay_up, decay_bias,
         span_shift, norm_gain):
    seqs, length, width = hidden.shape
    tok = seqs * length
    assert tok == 2 * BLOCK
    chips = n_dp // CORES
    depth = key_weight.shape[0]
    anywhere = pl.BlockSpec(memory_space=pl.ANY)
    vmem = pl.BlockSpec(memory_space=pltpu.VMEM)
    dma = pltpu.SemaphoreType.DMA
    result = pl.pallas_call(
        functools.partial(kernel, n_sp, n_dp),
        out_shape=jax.ShapeDtypeStruct((tok, VAL), bf16),
        in_specs=[anywhere] * 4 + [vmem] * 5,
        out_specs=anywhere,
        scratch_shapes=[
            pltpu.VMEM((HEADS, n_dp, depth, DK), bf16),
            pltpu.VMEM((tok, width), bf16),
            pltpu.VMEM((tok, KEY), bf16),
            pltpu.VMEM((tok, VAL), bf16),
            pltpu.VMEM((tok, VAL), bf16),
            pltpu.VMEM((tok, KEY), bf16),
            pltpu.VMEM((tok, KEY), bf16),
            pltpu.VMEM((tok, KEY), bf16),
            pltpu.VMEM((2, tok, KEY), bf16),
            pltpu.VMEM((5, tok, KEY), f32),
            pltpu.VMEM((1, KEY), f32),
            pltpu.VMEM((2, HEADS, DV, DK), f32),
            pltpu.VMEM((2, HEADS, SPLIT, DVS, DK), bf16),
            pltpu.VMEM((2, HEADS, SPLIT, DVS, DK), bf16),
            pltpu.VMEM((HEADS, tok, DV), f32),
            dma((HEADS + 3,)),
            dma((HEADS,)),
            dma((HEADS, chips)),
            dma((HEADS, chips)),
            dma((HEADS, chips)),
            dma((HEADS, chips)),
            dma((2, HEADS, SPLIT)),
            dma((2, HEADS, SPLIT)),
        ],
        compiler_params=pltpu.CompilerParams(
            collective_id=0, has_side_effects=True, vmem_limit_bytes=62 * 1024 * 1024),
    )(
        hidden.reshape(tok, width), queries.reshape(tok, KEY), values.reshape(tok, VAL),
        key_weight, decay_down.T, decay_up, decay_bias.reshape(1, KEY),
        span_shift.reshape(1, tok), norm_gain.reshape(1, VAL),
    )
    return result.reshape(seqs, length, VAL)


def solution(mesh):
    in_specs = (
        P("dp", "sp", None), P("dp", "sp", None), P("dp", "sp", None), P("dp", None),
        P(), P(), P(), P("dp", "sp"), P(),
    )
    return jax.shard_map(
        functools.partial(body, mesh.shape["sp"], mesh.shape["dp"]),
        mesh=mesh, in_specs=in_specs, out_specs=P("dp", "sp", None), check_vma=False)
```

```python
import functools

import jax
import jax.numpy as jnp
from jax import lax
from jax.experimental import pallas as pl
from jax.experimental.pallas import tpu as pltpu
from jax.sharding import PartitionSpec as P

HEADS = 4
DK = 256
DV = 512
BLOCK = 64
KEY = 1024
VAL = 2048
CORES = 2
SPLIT = 4
DVS = DV // SPLIT

decay_tau = 16.0
norm_eps = 1e-05
highest = lax.Precision.HIGHEST
MESH = pl.DeviceIdType.MESH
f32 = jnp.float32
bf16 = jnp.bfloat16


def each(low, high, fn):
    if high - low <= 4:
        for j in range(low, high):
            fn(j)
    else:
        lax.fori_loop(low, high, lambda j, c: (fn(j), c)[1], 0)


def dot_nt(a, b):
    return lax.dot_general(a, b, (((1,), (1,)), ((), ())), preferred_element_type=f32)


def dot_tn(a, b):
    return lax.dot_general(a, b, (((0,), (0,)), ((), ())), preferred_element_type=f32)


def kernel(
    n_sp, n_dp,
    hid, que, val, kw, down, up, bias, shift, gain,
    out,
    wbuf, hv, qv, vv, outv, qf, qb, qx, qs, fac, rate, local, sbuf, rbuf, acc,
    lsem, osem, wsend, wrecv, psend, precv, csend, crecv, dsend, drecv,
):
    sp = lax.axis_index("sp")
    dp = lax.axis_index("dp")
    chips = n_dp // CORES
    chip = dp // CORES
    core = dp % CORES
    partner = chip * CORES + (1 - core)
    tok = hv.shape[0]
    depth = kw.shape[0]

    square = chips == 4
    half = depth // 2

    def across(j):
        return (chip + 1 - 2 * lax.rem(chip, 2), lax.rem(chip + 2, 4), 3 - chip)[j - 1]

    def peer(j):
        if square:
            return across(j) * CORES + core
        return lax.rem(chip + j, chips) * CORES + core

    def source_chip(j):
        if square:
            return chip if j == 0 else across(j)
        return lax.rem(chip - j + chips, chips)

    wlocal = [
        pltpu.make_async_copy(kw.at[:, pl.ds(h * DK, DK)], wbuf.at[h, dp], lsem.at[h])
        for h in range(HEADS)
    ]
    inputs = [
        pltpu.make_async_copy(a, b, lsem.at[HEADS + i])
        for i, (a, b) in enumerate(((hid, hv), (que, qv), (val, vv)))
    ]
    for c in wlocal + inputs:
        c.start()

    barrier = pltpu.get_barrier_semaphore()
    each(1, chips, lambda j: pl.semaphore_signal(
        barrier, inc=1, device_id={"dp": peer(j)}, device_id_type=MESH))
    pl.semaphore_signal(barrier, inc=1, device_id={"dp": partner}, device_id_type=MESH)

    for side in (1, n_sp - 1):
        pl.semaphore_signal(
            barrier, inc=1, device_id={"sp": lax.rem(sp + side, n_sp)}, device_id_type=MESH)
    pl.semaphore_wait(barrier, chips + 2)

    def wcopy(h, j):
        return pltpu.make_async_remote_copy(
            src_ref=wbuf.at[h, dp], dst_ref=wbuf.at[h, dp],
            send_sem=wsend.at[h, j], recv_sem=wrecv.at[h, j],
            device_id={"dp": peer(j)}, device_id_type=MESH)

    def wland(h, j):
        slot = wbuf.at[h, source_chip(j) * CORES + core]
        return pltpu.make_async_remote_copy(
            src_ref=slot, dst_ref=slot,
            send_sem=wsend.at[h, j], recv_sem=wrecv.at[h, j],
            device_id={"dp": peer(j)}, device_id_type=MESH)

    def pcopy(h, j):
        slot = wbuf.at[h, source_chip(j) * CORES + core]
        return pltpu.make_async_remote_copy(
            src_ref=slot, dst_ref=slot,
            send_sem=psend.at[h, j], recv_sem=precv.at[h, j],
            device_id={"dp": partner}, device_id_type=MESH)

    def pland(h, j):
        slot = wbuf.at[h, source_chip(j) * CORES + (1 - core)]
        return pltpu.make_async_remote_copy(
            src_ref=slot, dst_ref=slot,
            send_sem=psend.at[h, j], recv_sem=precv.at[h, j],
            device_id={"dp": partner}, device_id_type=MESH)

    direct = 3 if square else chips

    def diagonal(h, i, lands):
        origin = source_chip(3) if lands else source_chip(1 + i)
        slot = wbuf.at[h, origin * CORES + core, pl.ds(i * half, half), :]
        return pltpu.make_async_remote_copy(
            src_ref=slot, dst_ref=slot,
            send_sem=dsend.at[h, i], recv_sem=drecv.at[h, i],
            device_id={"dp": peer(2 - i)}, device_id_type=MESH)

    def phase_send(h):
        wlocal[h].wait()
        each(1, direct, lambda j: wcopy(h, j).start())
        pcopy(h, 0).start()

    def phase_relay(h):
        def relay(j):
            wland(h, j).wait_recv()
            if square:
                diagonal(h, j - 1, False).start()
            pcopy(h, j).start()
        each(1, direct, relay)

    ahead = 2 if square else HEADS
    for h in range(ahead):
        phase_send(h)

    inputs[0].wait()
    low = dot_nt(hv[...], down[...]).astype(bf16)
    steps = shift[...].astype(f32)
    inputs[1].wait()
    row = lax.broadcasted_iota(jnp.int32, (tok, DK), 0)
    first = row < BLOCK
    ti = lax.broadcasted_iota(jnp.int32, (tok, tok), 0)
    tj = lax.broadcasted_iota(jnp.int32, (tok, tok), 1)
    same = (ti < BLOCK) == (tj < BLOCK)
    below = tj <= ti
    tri = jnp.where(same & below, 1.0, 0.0).astype(f32)
    def phase_prep(h):
        cols = pl.ds(h * DK, DK)
        pre = jnp.dot(low.astype(f32), up[:, cols], precision=highest, preferred_element_type=f32)
        pre = pre + bias[:, cols] + jnp.where(first, steps[:, :1], steps[:, BLOCK:BLOCK + 1])
        logd = (jnp.minimum(pre, 0.0) - jnp.log1p(jnp.exp(-jnp.abs(pre)))) * (1.0 / decay_tau)
        incl = jnp.dot(tri, logd, precision=highest, preferred_element_type=f32)
        excl = incl - logd
        t0 = incl[BLOCK - 1:BLOCK, :]
        t1 = incl[tok - 1:tok, :]
        here = jnp.where(first, t0, t1)
        after = jnp.where(first, t1, 0.0)
        before = jnp.where(first, 0.0, t0)
        scaled = qv[:, cols].astype(f32) * DK ** (-0.5)
        qf[:, cols] = (scaled * jnp.exp(incl)).astype(bf16)
        qb[:, cols] = (scaled * jnp.exp(-excl)).astype(bf16)
        qx[:, cols] = (scaled * jnp.exp(here - excl)).astype(bf16)
        qs[0, :, cols] = (scaled * jnp.exp(incl + before)).astype(bf16)
        qs[1, :, cols] = (scaled * jnp.exp(here - excl + after)).astype(bf16)
        fac[0, :, cols] = jnp.exp(-incl)
        fac[1, :, cols] = jnp.exp(excl)
        fac[2, :, cols] = jnp.exp(here - incl)
        fac[3, :, cols] = jnp.exp(here - incl + after)
        fac[4, :, cols] = jnp.exp(excl + before)
        rate[:, cols] = jnp.exp(t0 + t1)

    inputs[2].wait()

    def chain(way, h, s):
        target = jnp.clip(sp + 1 - 2 * way, 0, n_sp - 1)
        return pltpu.make_async_remote_copy(
            src_ref=sbuf.at[way, h, s], dst_ref=rbuf.at[way, h, s],
            send_sem=csend.at[way, h, s], recv_sem=crecv.at[way, h, s],
            device_id={"sp": target}, device_id_type=MESH)

    def phase_keys(h):
        if square:
            for i in range(2):
                diagonal(h, i, True).wait_recv()
            pcopy(h, 3).start()
        each(0, chips, lambda j: pland(h, j).wait_recv())
        cols = pl.ds(h * DK, DK)
        weights = wbuf[h].reshape(n_dp * depth, DK)
        keys = jnp.dot(hv[...], weights, preferred_element_type=f32).astype(bf16).astype(f32)
        v = vv[:, pl.ds(h * DV, DV)]
        k_fwd = (keys * fac[3, :, cols]).astype(bf16)
        k_bwd = (keys * fac[4, :, cols]).astype(bf16)
        for way, k in ((0, k_fwd), (1, k_bwd)):
            local[way, h] = dot_tn(v, k)

            @pl.when(sp == (0 if way == 0 else n_sp - 1))
            def _(way=way):
                for s in range(SPLIT):
                    sbuf[way, h, s] = local[way, h, pl.ds(s * DVS, DVS), :].astype(bf16)
                    chain(way, h, s).start()

        kf = (keys * fac[0, :, cols]).astype(bf16)
        kb = (keys * fac[1, :, cols]).astype(bf16)
        ke = (keys * fac[2, :, cols]).astype(bf16)
        query_f, query_b, query_x = qf[:, cols], qb[:, cols], qx[:, cols]
        lower = jnp.where(same, dot_nt(query_f, kf), dot_nt(query_f, ke))
        upper = jnp.where(same, dot_nt(query_b, kb), dot_nt(query_x, kb))
        scores = jnp.where(below, lower, upper).astype(bf16)
        acc[h] = jnp.dot(scores, v, preferred_element_type=f32)

    def phase_chain(way, h):
        cols = pl.ds(h * DK, DK)
        edge = way * (n_sp - 1)
        other = (1 - way) * (n_sp - 1)

        @pl.when(sp != edge)
        def _():
            for s in range(SPLIT):
                rows = pl.ds(s * DVS, DVS)
                chain(way, h, s).wait_recv()

                @pl.when(sp != other)
                def _(s=s, rows=rows):
                    state = rbuf[way, h, s].astype(f32) * rate[:, cols] + local[way, h, rows, :]
                    sbuf[way, h, s] = state.astype(bf16)
                    chain(way, h, s).start()

                acc[h, :, rows] += dot_nt(qs[way, :, cols], rbuf[way, h, s])

    def out_copy(h):
        cols = pl.ds(h * DV, DV)
        return pltpu.make_async_copy(outv.at[:, cols], out.at[:, cols], osem.at[h])

    def phase_out(h):
        cols = pl.ds(h * DV, DV)
        mixed = acc[h].astype(bf16).astype(f32)
        scale = lax.rsqrt(jnp.mean(mixed * mixed, axis=-1, keepdims=True) + norm_eps)
        outv[:, cols] = (mixed * scale * gain[:, cols]).astype(bf16)
        out_copy(h).start()

    near = jnp.where(sp * 2 < n_sp, 0, 1)
    far = 1 - near
    def relay_on(h):
        if h < HEADS:
            phase_relay(h)
            if h + ahead < HEADS:
                phase_send(h + ahead)

    def phase_near(h):
        phase_chain(near, h)

    def phase_far(h):
        phase_chain(far, h)
        phase_out(h)

    plan = ((phase_prep, 0), (relay_on, 0), (phase_prep, 1), (relay_on, 1), (phase_keys, 0), (phase_prep, 2), (relay_on, 2), (phase_keys, 1), (phase_prep, 3), (relay_on, 3), (phase_keys, 2), (phase_near, 0), (phase_keys, 3), (phase_near, 1), (phase_far, 0), (phase_near, 2), (phase_far, 1), (phase_near, 3), (phase_far, 2), (phase_far, 3))
    for phase, h in plan:
        phase(h)

    for h in range(HEADS):
        each(1, direct, lambda j, h=h: wcopy(h, j).wait_send())
        each(0, chips, lambda j, h=h: pcopy(h, j).wait_send())
        if square:
            for i in range(2):
                diagonal(h, i, False).wait_send()
        for way in range(2):
            @pl.when(sp != (1 - way) * (n_sp - 1))
            def _(h=h, way=way):
                for s in range(SPLIT):
                    chain(way, h, s).wait_send()
        out_copy(h).wait()


def body(n_sp, n_dp, hidden, queries, values, key_weight, decay_down, decay_up, decay_bias,
         span_shift, norm_gain):
    seqs, length, width = hidden.shape
    tok = seqs * length
    assert tok == 2 * BLOCK
    chips = n_dp // CORES
    depth = key_weight.shape[0]
    anywhere = pl.BlockSpec(memory_space=pl.ANY)
    vmem = pl.BlockSpec(memory_space=pltpu.VMEM)
    dma = pltpu.SemaphoreType.DMA
    result = pl.pallas_call(
        functools.partial(kernel, n_sp, n_dp),
        out_shape=jax.ShapeDtypeStruct((tok, VAL), bf16),
        in_specs=[anywhere] * 4 + [vmem] * 5,
        out_specs=anywhere,
        scratch_shapes=[
            pltpu.VMEM((HEADS, n_dp, depth, DK), bf16),
            pltpu.VMEM((tok, width), bf16),
            pltpu.VMEM((tok, KEY), bf16),
            pltpu.VMEM((tok, VAL), bf16),
            pltpu.VMEM((tok, VAL), bf16),
            pltpu.VMEM((tok, KEY), bf16),
            pltpu.VMEM((tok, KEY), bf16),
            pltpu.VMEM((tok, KEY), bf16),
            pltpu.VMEM((2, tok, KEY), bf16),
            pltpu.VMEM((5, tok, KEY), f32),
            pltpu.VMEM((1, KEY), f32),
            pltpu.VMEM((2, HEADS, DV, DK), f32),
            pltpu.VMEM((2, HEADS, SPLIT, DVS, DK), bf16),
            pltpu.VMEM((2, HEADS, SPLIT, DVS, DK), bf16),
            pltpu.VMEM((HEADS, tok, DV), f32),
            dma((HEADS + 3,)),
            dma((HEADS,)),
            dma((HEADS, chips)),
            dma((HEADS, chips)),
            dma((HEADS, chips)),
            dma((HEADS, chips)),
            dma((2, HEADS, SPLIT)),
            dma((2, HEADS, SPLIT)),
            dma((HEADS, 2)),
            dma((HEADS, 2)),
        ],
        compiler_params=pltpu.CompilerParams(
            collective_id=0, has_side_effects=True, vmem_limit_bytes=62 * 1024 * 1024),
    )(
        hidden.reshape(tok, width), queries.reshape(tok, KEY), values.reshape(tok, VAL),
        key_weight, decay_down.T, decay_up, decay_bias.reshape(1, KEY),
        span_shift.reshape(1, tok), norm_gain.reshape(1, VAL),
    )
    return result.reshape(seqs, length, VAL)


def solution(mesh):
    in_specs = (
        P("dp", "sp", None), P("dp", "sp", None), P("dp", "sp", None), P("dp", None),
        P(), P(), P(), P("dp", "sp"), P(),
    )
    return jax.shard_map(
        functools.partial(body, mesh.shape["sp"], mesh.shape["dp"]),
        mesh=mesh, in_specs=in_specs, out_specs=P("dp", "sp", None), check_vma=False)
```
